256 devices in a mesh: grp: 2 (over z), sp: 64 (over y, x), tp: 2 (over core).
Axes of the slice: x: 8, y: 8, z: 2, core: 2. Of those that a mesh axis runs over, the one named last changes fastest.
The devices are a block of a 8x8x16 slice.
Arguments:
- tokens: bfloat16 [65536, 2048], P(('grp', 'sp', 'tp')), parts along dimension 0, may hold values from -64 to 64
- w_query: bfloat16 [2048, 1024], P(None, 'tp'), may hold values from -0.125 to 0.125
- w_key: bfloat16 [2048, 1024], P(None, 'tp'), may hold values from -0.125 to 0.125
- w_value: bfloat16 [2048, 1024], P(None, 'tp'), may hold values from -0.25 to 0.25
- w_out: bfloat16 [1024, 2048], P('tp'), may hold values from -0.1875 to 0.1875
Outputs:
- mixed: bfloat16 [65536, 2048], P(('grp', 'sp', 'tp')), parts along dimension 0
- log_sums: float32 [16, 65536], P('tp', ('grp', 'sp')), parts along dimension 1
The draws below stay inside these ranges and needn't reach their ends.
There are 2 independent parts, one for each index of `grp`. The reference program is written for one: setup_inputs(seed, part) draws one part's arguments, and reference() takes and returns one part's arrays. A program takes and returns all parts, laid end to end along the dimension named above; an argument that names none is the same for every part. Nothing has to cross between parts.
All inputs are finite; a program needn't handle non-finite values.
Results may differ from the reference program's by a relative error of at most 0.013.
The reference program's roundings to bfloat16 on the way count: a program that leaves them out, or rounds other values in their place, can miss the bound.
Values may be sent and summed in bfloat16 or wider, within the bound.
A program may use at most 128 MiB of HBM per device.

```python
import math
import jax
import jax.numpy as jnp
from jax import lax

D = 2048
HEADS = 16
HEAD_DIM = 64
WINDOW_KEY_STEPS = 128
MIDDLE_DILATION = 4
FAR_DILATION = 16
TOK_DEV = 512
TOKENS = 32768
REACH = 2048
N_SP = 64
N_TP = 2


def draw_tokens(key, part):
    base = jnp.clip(jax.random.normal(jax.random.fold_in(key, 11), (TOKENS, D), jnp.float32), -4.0, 4.0)
    return base.astype(jnp.bfloat16)


def block_levels(own_key, dims, split, least, largest):
    loudness = 1.0
    for position, shards_of in split:
        steps = jax.random.uniform(jax.random.fold_in(jax.random.fold_in(own_key, 6), position), (shards_of,), jnp.float32, least / len(split), largest / len(split))
        loudness = loudness * jnp.repeat(jnp.exp(steps), dims[position] // shards_of).reshape((-1,) + (1,) * (len(dims) - 1 - position))
    return loudness


def bell_draw(key, dims, scale, bound, split=(), kind=jnp.bfloat16):
    result = scale * jax.random.normal(key, dims, jnp.float32)
    if split:
        result = result * block_levels(key, dims, split, -0.22, 0.18)
    return jnp.clip(result, -bound, bound).astype(kind)


def setup_inputs(seed: int = 0, part: int = 0) -> dict:
    key_list = jax.random.split(jax.random.key(seed), 6)
    part_splits = jax.random.split(jax.random.fold_in(key_list[5], part), 6)
    tokens = draw_tokens(jax.random.fold_in(jax.random.fold_in(key_list[5], part), 71), part)
    w_query = bell_draw(key_list[1], (D, HEADS * HEAD_DIM), D ** -0.5, 0.125, ((1, 2),))
    w_key = bell_draw(key_list[2], (D, HEADS * HEAD_DIM), D ** -0.5, 0.125, ((1, 2),))
    w_value = bell_draw(key_list[3], (D, HEADS * HEAD_DIM), (D // 4) ** -0.5, 0.25, ((1, 2),))
    w_out = bell_draw(key_list[4], (HEADS * HEAD_DIM, D), (HEADS * HEAD_DIM) ** -0.5, 0.1875, ((0, 2),))
    return dict(tokens=tokens, w_query=w_query, w_key=w_key, w_value=w_value, w_out=w_out)


ALIBI_EXP = 16.0


def dilated_attention(query_rows, key_value_rows, dilation, window_steps, head_slopes, first_position):
    length, heads, depth = query_rows.shape
    total_rows = key_value_rows.shape[0]
    strided = length // dilation
    block_rows = math.gcd(strided, 128)
    num_blocks = strided // block_rows
    behind = (total_rows - length) // dilation
    grouped = query_rows.reshape(num_blocks, block_rows, dilation, heads, depth)
    columns = key_value_rows.reshape(total_rows // dilation, dilation, 2, heads, depth)
    spans = jnp.stack([columns[behind + index * block_rows - window_steps: behind + (index + 1) * block_rows]
                       for index in range(num_blocks)])
    scores = jnp.einsum("bqrhe,bkrhe->brhqk", grouped.astype(jnp.float32),
                        spans[:, :, :, 0].astype(jnp.float32)) * depth ** -0.5
    row_pos = jnp.arange(block_rows, dtype=jnp.int32)[:, None]
    key_pos = jnp.arange(window_steps + block_rows, dtype=jnp.int32)[None, :]
    distance = window_steps + row_pos - key_pos
    inside = (distance >= 0) & (distance <= window_steps)
    block_pos = jnp.arange(num_blocks, dtype=jnp.int32)[:, None, None, None]
    residue = jnp.arange(dilation, dtype=jnp.int32)[None, :, None, None]
    source = first_position + (block_pos * block_rows - window_steps + key_pos[None, None]) * dilation + residue
    allowed = inside[None, None] & (source >= 0)
    penalty = -head_slopes[:, None, None] * (distance * dilation).astype(jnp.float32)
    scores = jnp.where(allowed[:, :, None], scores + penalty[None, None], -jnp.inf)
    maxima = jnp.max(scores, axis=-1, keepdims=True)
    weights = jnp.exp(scores - maxima)
    totals = jnp.sum(weights, axis=-1, keepdims=True)
    rounded = lax.optimization_barrier(weights.astype(jnp.bfloat16))
    summed = jnp.einsum("brhqk,bkrhe->bqrhe", rounded.astype(jnp.float32), spans[:, :, :, 1].astype(jnp.float32))
    outputs = summed / jnp.transpose(totals, (0, 3, 1, 2, 4))
    log_part = jnp.transpose((maxima + jnp.log(totals))[..., 0], (0, 3, 1, 2))
    return outputs.reshape(length, heads, depth), log_part.reshape(length, heads)


def combine(query_rows, key_value_rows, head_slopes, first_position):
    length, heads, depth = query_rows.shape
    window_results = [dilated_attention(query_rows, key_value_rows, window_stride, WINDOW_KEY_STEPS, head_slopes, first_position) for window_stride in (1, MIDDLE_DILATION, FAR_DILATION)]
    stacked = jnp.stack([item[1] for item in window_results])
    log_total = jax.nn.logsumexp(stacked, axis=0)
    hidden = jnp.zeros((length, heads, depth), jnp.float32)
    for item in window_results:
        hidden = hidden + jnp.exp(item[1] - log_total)[..., None] * item[0]
    return hidden.reshape(length, heads * depth).astype(jnp.bfloat16), log_total


def reference(tokens, w_query, w_key, w_value, w_out):
    query_rows = jnp.dot(tokens, w_query, preferred_element_type=jnp.float32).astype(jnp.bfloat16)
    keys = jnp.dot(tokens, w_key, preferred_element_type=jnp.float32).astype(jnp.bfloat16)
    values = jnp.dot(tokens, w_value, preferred_element_type=jnp.float32).astype(jnp.bfloat16)
    key_value_rows = jnp.concatenate([keys, values], axis=1)
    padded = jnp.concatenate([jnp.zeros((REACH, key_value_rows.shape[1]), jnp.bfloat16), key_value_rows], axis=0)
    head_slopes = jnp.exp2(-ALIBI_EXP * jnp.arange(1, HEADS + 1, dtype=jnp.float32) / HEADS)

    def segment(index):
        first = index * TOK_DEV
        query_seg = lax.dynamic_slice_in_dim(query_rows, first, TOK_DEV, 0).reshape(TOK_DEV, HEADS, HEAD_DIM)
        keyval_seg = lax.dynamic_slice_in_dim(padded, first, REACH + TOK_DEV, 0)
        return combine(query_seg, keyval_seg, head_slopes, first)

    hidden, log_total = lax.map(segment, jnp.arange(N_SP, dtype=jnp.int32))
    hidden = hidden.reshape(TOKENS, HEADS * HEAD_DIM)
    log_total = log_total.reshape(TOKENS, HEADS)
    width = HEADS * HEAD_DIM // N_TP
    mixed = jnp.zeros((TOKENS, D), jnp.float32)
    for group in range(N_TP):
        partial_value = jnp.dot(hidden[:, group * width:(group + 1) * width], w_out[group * width:(group + 1) * width],
                          preferred_element_type=jnp.float32).astype(jnp.bfloat16)
        mixed = mixed + lax.optimization_barrier(partial_value).astype(jnp.float32)
    return mixed.astype(jnp.bfloat16), log_total.T
```

```python
import functools

import jax
import jax.numpy as jnp
from jax import lax
from jax.experimental import pallas as pl
from jax.experimental.pallas import tpu as pltpu
from jax.sharding import PartitionSpec as P

HEADS = 16
HEAD_DIM = 64
STEPS = 128
REACH = 2048
ALIBI_EXP = 16.0
STRIDE = 16
LANES = 128
MASKED = -1e30
MESH = pl.DeviceIdType.MESH
F32 = jnp.float32
BF16 = jnp.bfloat16


def iota(shape, dim):
    return lax.broadcasted_iota(jnp.int32, shape, dim)


def permuted(m):
    return (m // LANES) * LANES + (m % 8) * STRIDE + (m % LANES) // 8


def kernel(
    rows_sp, tok, wq, wk, wv, wo, mixed, logs,
    x_in, x_perm, q_w, k_w, v_w, o_w, k_tmp, send_kv, send_q, kv, kv1, q_pk, q_near, q_far, k_far, k_far1,
    bias, far_r, far_m, mid_r, mid_m, o_send, o_recv, l_send, l_recv, l_nat, hid, part, other,
    load_sem, tok_sem, kv_s, kv_r, q_s, q_r, halo_s, halo_r, o_s, o_r, l_s, l_r, part_s, part_r, in_sem,
):
    half, depth = tok.shape
    block = 2 * half
    group = q_w.shape[1] // HEAD_DIM
    halo = REACH // block
    far_rows = block // STRIDE
    sp, tp = lax.axis_index("sp"), lax.axis_index("tp")
    x = lax.rem(sp, group)
    base = sp - x
    y = sp // group
    up = rows_sp - 1

    def peer(d):
        return {"sp": base + d, "tp": tp}

    partner = {"tp": 1 - tp}

    mine = pl.multiple_of(tp * half, half)
    loads = [
        pltpu.make_async_copy(tok, x_in.at[pl.ds(mine, half)], load_sem.at[0]),
        pltpu.make_async_copy(wk, k_w, load_sem.at[1]),
        pltpu.make_async_copy(wv, v_w, load_sem.at[2]),
        pltpu.make_async_copy(wq, q_w, load_sem.at[3]),
        pltpu.make_async_copy(wo, o_w, load_sem.at[4]),
    ]
    for c in loads:
        c.start()

    barrier = pltpu.get_barrier_semaphore()
    pl.semaphore_signal(barrier, inc=1, device_id=partner, device_id_type=MESH)
    for d in range(group):
        @pl.when(d < x)
        def _():
            pl.semaphore_signal(barrier, inc=1, device_id=peer(d), device_id_type=MESH)

    @pl.when(y > 0)
    def _():
        pl.semaphore_signal(barrier, inc=1, device_id={"sp": sp - group, "tp": tp}, device_id_type=MESH)

    head = (tp * group + x + 1).astype(F32)
    slope = jnp.exp2(jnp.full((LANES, 2 * LANES), -ALIBI_EXP / HEADS, F32) * head)
    row, col = iota((LANES, 2 * LANES), 0), iota((LANES, 2 * LANES), 1)
    near_d = STEPS + permuted(row) - (col // LANES) * LANES - permuted(col % LANES)
    mid_d = STEPS + 4 * (row % 32) + row // 32 - ((col % 64) // 32) * LANES - 4 * (col % 32) - col // 64
    far_d = STEPS + row - col
    before = (col < LANES, (col % 64) < 32, col < LANES)
    for w, (dist, stride) in enumerate(((near_d, 1), (mid_d, 4), (far_d, 16))):
        plain = jnp.where((dist >= 0) & (dist <= STEPS), -slope * (dist * stride).astype(F32), MASKED)
        bias[2 * w] = plain
        bias[2 * w + 1] = jnp.where(before[w] & (y == 0), MASKED, plain)

    low = iota((half, LANES), 1) < HEAD_DIM

    @pl.when(y == 0)
    def _():
        kv[pl.ds(0, REACH), :] = jnp.zeros((REACH, LANES), BF16)

    pl.semaphore_wait(barrier, group - x + jnp.where(y < up, 1, 0))
    for d in range(group):
        @pl.when(d > x)
        def _():
            pl.semaphore_signal(in_sem.at[x], inc=1, device_id=peer(d), device_id_type=MESH)

    loads[0].wait()
    tok_copy = pltpu.make_async_remote_copy(
        src_ref=x_in.at[pl.ds(mine, half)], dst_ref=x_in.at[pl.ds(mine, half)],
        send_sem=tok_sem.at[0], recv_sem=tok_sem.at[1], device_id=partner, device_id_type=MESH)
    tok_copy.start()
    pm, pt = iota((half, half), 0), iota((half, half), 1)
    perm = jnp.where(permuted(pm) == pt, 1.0, 0.0).astype(BF16)
    back = jnp.where(permuted(pt) == pm, 1.0, 0.0).astype(BF16)

    def permute(first):
        x_perm[pl.ds(first, half), :] = jnp.dot(perm, x_in[pl.ds(first, half), :], preferred_element_type=F32).astype(BF16)

    permute(mine)
    other_half = pl.multiple_of((1 - tp) * half, half)
    their_copy = pltpu.make_async_remote_copy(
        src_ref=x_in.at[pl.ds(mine, half)], dst_ref=x_in.at[pl.ds(other_half, half)],
        send_sem=tok_sem.at[0], recv_sem=tok_sem.at[1], device_id=partner, device_id_type=MESH)
    their_copy.wait_recv()
    permute(other_half)

    def kv_copy(d, source):
        return pltpu.make_async_remote_copy(
            src_ref=send_kv.at[d], dst_ref=kv.at[pl.ds(pl.multiple_of(REACH + source * block, block), block)],
            send_sem=kv_s.at[d], recv_sem=kv_r.at[source], device_id=peer(d), device_id_type=MESH)

    def q_copy(d, source):
        return pltpu.make_async_remote_copy(
            src_ref=send_q.at[d], dst_ref=q_pk.at[source],
            send_sem=q_s.at[d], recv_sem=q_r.at[source], device_id=peer(d), device_id_type=MESH)

    own_kv = pltpu.make_async_copy(send_kv.at[x], kv.at[pl.ds(pl.multiple_of(REACH + x * block, block), block)], kv_s.at[x])
    own_q = pltpu.make_async_copy(send_q.at[x], q_pk.at[x], q_s.at[x])

    for c in loads[1:4]:
        c.wait()
    wide = 2 * LANES
    heads_at_once = wide // HEAD_DIM
    low_block = iota((block, LANES), 1) < HEAD_DIM
    order = (4, 3, 5, 2, 6, 1, 7)
    for g in reversed(range(group // heads_at_once)):
        cols = slice(g * wide, (g + 1) * wide)
        k_tmp[...] = jnp.dot(x_perm[...], k_w[:, cols], preferred_element_type=F32)
        v_all = jnp.dot(x_perm[...], v_w[:, cols], preferred_element_type=F32)
        for p in range(2):
            k_p, v_p = k_tmp[:, p * LANES:(p + 1) * LANES], v_all[:, p * LANES:(p + 1) * LANES]
            d = g * heads_at_once + 2 * p
            send_kv[d] = jnp.where(low_block, k_p, pltpu.roll(v_p, HEAD_DIM, 1)).astype(BF16)
            send_kv[d + 1] = jnp.where(low_block, pltpu.roll(k_p, HEAD_DIM, 1), v_p).astype(BF16)
        q_all = jnp.dot(x_perm[...], q_w[:, cols], preferred_element_type=F32) * HEAD_DIM ** -0.5
        for p in range(2):
            q_a, q_b = q_all[:half, p * LANES:(p + 1) * LANES], q_all[half:, p * LANES:(p + 1) * LANES]
            d = g * heads_at_once + 2 * p
            send_q[d] = jnp.where(low, q_a, pltpu.roll(q_b, HEAD_DIM, 1)).astype(BF16)
            send_q[d + 1] = jnp.where(low, pltpu.roll(q_a, HEAD_DIM, 1), q_b).astype(BF16)
        for step in order:
            d = lax.rem(x + step, group)

            @pl.when((d // heads_at_once == g) & (d > 0))
            def _():
                @pl.when(d < x)
                def _():
                    pl.semaphore_wait(in_sem.at[d], 1)

                kv_copy(d, x).start()
                q_copy(d, x).start()

        @pl.when(x // heads_at_once == g)
        def _():
            own_kv.start()
            own_q.start()

    @pl.when(x > 0)
    def _():
        pl.semaphore_wait(in_sem.at[0], 1)
        kv_copy(0, x).start()
        q_copy(0, x).start()

    lane_low = iota((half, LANES), 1) < HEAD_DIM

    def to_far(ref, values, slot, part_index):
        for r in range(STRIDE):
            pair = jnp.concatenate([values[8 * r:8 * r + 8], values[LANES + 8 * r:LANES + 8 * r + 8]], axis=0)
            ref[r, pl.ds(pl.multiple_of(far_rows * slot + 16 * part_index, 16), 16), :] = pair.astype(BF16)

    def take_keys(slot):
        for h in range(2):
            first = pl.multiple_of(slot * block + h * half, half)
            values = kv[pl.ds(first, half), :].astype(F32)
            with_ones = jnp.where(lane_low, 1.0, values)
            kv1[pl.ds(first, half), :] = with_ones.astype(BF16)
            to_far(k_far, values, slot, h)
            to_far(k_far1, with_ones, slot, h)

    def take_queries(b):
        values = q_pk[b].astype(F32)
        for h in range(2):
            part_q = jnp.where(lane_low, values if h == 0 else pltpu.roll(values, HEAD_DIM, 1), 0.0)
            q_near[pl.ds(pl.multiple_of(b * block + h * half, half), half), :] = part_q.astype(BF16)
            to_far(q_far, part_q, b, h)

    def halo_copy(b):
        return pltpu.make_async_remote_copy(
            src_ref=kv.at[pl.ds(pl.multiple_of(REACH + b * block, block), block)],
            dst_ref=kv.at[pl.ds(pl.multiple_of((b - (group - halo)) * block, block), block)],
            send_sem=halo_s.at[b - (group - halo)], recv_sem=halo_r.at[b - (group - halo)],
            device_id={"sp": sp + group, "tp": tp}, device_id_type=MESH)

    def pass_on(b):
        @pl.when((b >= group - halo) & (y < up))
        def _():
            halo_copy(b).start()

    own_kv.wait()
    own_q.wait()
    pass_on(x)
    take_keys(x + halo)
    take_queries(x)

    def arrive(i, carry):
        b = lax.rem(x + i, group)
        kv_copy(b, b).wait_recv()
        pass_on(b)
        take_keys(b + halo)
        q_copy(b, b).wait_recv()
        take_queries(b)
        return carry

    lax.fori_loop(1, group, arrive, 0)

    def take_halo(i, carry):
        @pl.when(y > 0)
        def _():
            halo_copy(i + group - halo).wait_recv()

        take_keys(i)
        return carry

    lax.fori_loop(0, halo, take_halo, 0)

    def scores(q, keys, which):
        s = lax.dot_general(q, keys, (((1,), (1,)), ((), ())), preferred_element_type=F32) + bias[which]
        m = jnp.max(s, axis=1, keepdims=True)
        return jnp.exp(s - m).astype(BF16), m

    first_row = jnp.where(y == 0, 1, 0)
    eights = [(c, pl.ds(8 * c, 8)) for c in range(LANES // 8)]

    def far_step(i, carry):
        for rr in range(2):
            r = 2 * i + rr
            for qb in range(group * far_rows // LANES):
                keys = pl.ds(qb * LANES, 2 * LANES)
                w, m = scores(q_far[r, pl.ds(qb * LANES, LANES), :], k_far[r, keys, :], 4 + (1 if qb == 0 else 0))
                res = jnp.dot(w, k_far1[r, keys, :], preferred_element_type=F32)
                m_all = jnp.broadcast_to(m, (LANES, LANES))
                for c in range(LANES // 8):
                    dst = (qb * (LANES // far_rows) + c // 4) * block + (c % 4) * LANES
                    at = pl.ds(pl.multiple_of(dst + 8 * r, 8), 8)
                    far_r[at, :] = res[8 * c:8 * c + 8]
                    far_m[at, :] = m_all[8 * c:8 * c + 8]
        return carry

    lax.fori_loop(0, STRIDE // 2, far_step, 0)

    def mid_step(b, carry):
        which = 2 + jnp.where(b == 0, first_row, 0)
        for rho in range(4):
            rows_q = pl.ds(pl.multiple_of(far_rows * b, far_rows), far_rows)
            rows_k = pl.ds(pl.multiple_of(far_rows * (b + halo - 1), far_rows), 2 * far_rows)
            q = jnp.concatenate([q_far[rho + 4 * s, rows_q, :] for s in range(4)], axis=0)
            keys = jnp.concatenate([k_far[rho + 4 * s, rows_k, :] for s in range(4)], axis=0)
            keys1 = jnp.concatenate([k_far1[rho + 4 * s, rows_k, :] for s in range(4)], axis=0)
            w, m = scores(q, keys, which)
            res = jnp.dot(w, keys1, preferred_element_type=F32)
            m_all = jnp.broadcast_to(m, (LANES, LANES))
            for c in range(LANES // 8):
                at = pl.ds(pl.multiple_of(b * block + (c % 4) * LANES + 8 * (rho + 4 * (c // 4)), 8), 8)
                mid_r[at, :] = res[8 * c:8 * c + 8]
                mid_m[at, :] = m_all[8 * c:8 * c + 8]
        return carry

    lax.fori_loop(0, group, mid_step, 0)

    def o_copy(d, source):
        return pltpu.make_async_remote_copy(
            src_ref=o_send.at[d], dst_ref=o_recv.at[source],
            send_sem=o_s.at[d], recv_sem=o_r.at[source], device_id=peer(d), device_id_type=MESH)

    def l_copy(d, source):
        return pltpu.make_async_remote_copy(
            src_ref=l_send.at[d], dst_ref=l_recv.at[source],
            send_sem=l_s.at[d], recv_sem=l_r.at[source], device_id=peer(d), device_id_type=MESH)

    square_low = iota((LANES, LANES), 1) < HEAD_DIM
    eye = iota((LANES, LANES), 0) == iota((LANES, LANES), 1)

    def near_step(i, carry):
        b = lax.rem(x + i + group // 2, group)
        for a2 in range(2):
            pieces = []
            for a in (a2, a2 + 2):
                at = pl.ds(pl.multiple_of(b * block + a * LANES, LANES), LANES)
                keys = pl.ds(pl.multiple_of(REACH + b * block + (a - 1) * LANES, LANES), 2 * LANES)
                w, m = scores(q_near[at, :], kv[keys, :], jnp.where(b == 0, first_row, 0) if a == 0 else 0)
                res = jnp.dot(w, kv1[keys, :], preferred_element_type=F32)
                m_f, m_m = far_m[at, :], mid_m[at, :]
                top = jnp.maximum(jnp.maximum(m_f, m_m), m)
                den = jnp.exp(m - top) * res + jnp.exp(m_f - top) * far_r[at, :] + jnp.exp(m_m - top) * mid_r[at, :]
                turned = pltpu.roll(den, HEAD_DIM, 1)
                total = jnp.where(square_low, den, turned)
                l_send[b, a, :] = jnp.sum(jnp.where(eye, top + jnp.log(total), 0.0), axis=0)
                pieces.append((turned if a < 2 else den) / total)
            o_send[b, pl.ds(a2 * LANES, LANES), :] = jnp.where(square_low, pieces[0], pieces[1]).astype(BF16)

        @pl.when(b != x)
        def _():
            o_copy(b, x).start()
            l_copy(b, x).start()

        return carry

    lax.fori_loop(0, group, near_step, 0)
    own_o = pltpu.make_async_copy(o_send.at[x], o_recv.at[x], o_s.at[x])
    own_l = pltpu.make_async_copy(l_send.at[x], l_recv.at[x], l_s.at[x])
    own_o.start()
    own_l.start()
    own_o.wait()
    own_l.wait()

    def returned(i, carry):
        b = lax.rem(x + i, group)
        o_copy(b, b).wait_recv()
        l_copy(b, b).wait_recv()
        return carry

    lax.fori_loop(1, group, returned, 0)

    for p in range(group // 2):
        even, odd = o_recv[2 * p].astype(F32), o_recv[2 * p + 1].astype(F32)
        cols = slice(p * LANES, (p + 1) * LANES)
        first = jnp.where(low, even, pltpu.roll(odd, HEAD_DIM, 1)).astype(BF16)
        second = jnp.where(low, pltpu.roll(even, HEAD_DIM, 1), odd).astype(BF16)
        hid[:half, cols] = jnp.dot(back, first, preferred_element_type=F32).astype(BF16)
        hid[half:, cols] = jnp.dot(back, second, preferred_element_type=F32).astype(BF16)
    loads[4].wait()

    pieces_out = part.shape[0]
    step_cols = depth // pieces_out

    def part_copy(i):
        return pltpu.make_async_remote_copy(
            src_ref=part.at[i], dst_ref=other.at[i], send_sem=part_s.at[i], recv_sem=part_r.at[i],
            device_id=partner, device_id_type=MESH)

    for i in range(pieces_out):
        part[i] = jnp.dot(hid[pl.ds(other_half, half), :], o_w[:, i * step_cols:(i + 1) * step_cols],
                          preferred_element_type=F32).astype(BF16)
        part_copy(i).start()

    flat = jnp.concatenate([l_recv[h] for h in range(group)], axis=0)
    l_nat[...] = jnp.dot(flat, perm[:LANES, :LANES].astype(F32), preferred_element_type=F32, precision=lax.Precision.HIGHEST)
    for a in range(block // LANES):
        logs[:, a * LANES:(a + 1) * LANES] = l_nat[pl.ds(a, group, stride=8), :]

    for i in range(pieces_out):
        own = jnp.dot(hid[pl.ds(mine, half), :], o_w[:, i * step_cols:(i + 1) * step_cols],
                      preferred_element_type=F32).astype(BF16)
        part_copy(i).wait_recv()
        mixed[:, i * step_cols:(i + 1) * step_cols] = (own.astype(F32) + other[i].astype(F32)).astype(BF16)

    tok_copy.wait_send()
    for d in range(group):
        @pl.when(d != x)
        def _():
            kv_copy(d, x).wait_send()
            q_copy(d, x).wait_send()
            o_copy(d, x).wait_send()
            l_copy(d, x).wait_send()

    for i in range(halo):
        @pl.when(y < up)
        def _():
            halo_copy(i + group - halo).wait_send()

    for i in range(pieces_out):
        part_copy(i).wait_send()


def solution(mesh):
    def body(tokens, w_query, w_key, w_value, w_out):
        half, depth = tokens.shape
        width = w_query.shape[1]
        block, group = 2 * half, width // HEAD_DIM
        halo = REACH // block
        length = group * block
        far_rows = block // STRIDE
        pieces_out = 4
        vmem = pltpu.VMEM
        dma = pltpu.SemaphoreType.DMA
        anywhere = pl.BlockSpec(memory_space=pl.ANY)
        return pl.pallas_call(
            functools.partial(kernel, mesh.shape["sp"] // group),
            name="attention_layer",
            out_shape=(
                jax.ShapeDtypeStruct((half, depth), BF16),
                jax.ShapeDtypeStruct((group, block), F32),
            ),
            in_specs=[anywhere] * 5,
            out_specs=(pl.BlockSpec(memory_space=vmem), pl.BlockSpec(memory_space=vmem)),
            scratch_shapes=[
                vmem((block, depth), BF16),
                vmem((block, depth), BF16),
                vmem((depth, width), BF16),
                vmem((depth, width), BF16),
                vmem((depth, width), BF16),
                vmem((width, depth), BF16),
                vmem((block, 2 * LANES), F32),
                vmem((group, block, LANES), BF16),
                vmem((group, half, LANES), BF16),
                vmem((REACH + length, LANES), BF16),
                vmem((REACH + length, LANES), BF16),
                vmem((group, half, LANES), BF16),
                vmem((length, LANES), BF16),
                vmem((STRIDE, group * far_rows, LANES), BF16),
                vmem((STRIDE, (halo + group) * far_rows, LANES), BF16),
                vmem((STRIDE, (halo + group) * far_rows, LANES), BF16),
                vmem((6, LANES, 2 * LANES), F32),
                vmem((length, LANES), F32),
                vmem((length, LANES), F32),
                vmem((length, LANES), F32),
                vmem((length, LANES), F32),
                vmem((group, half, LANES), BF16),
                vmem((group, half, LANES), BF16),
                vmem((group, 8, LANES), F32),
                vmem((group, 8, LANES), F32),
                vmem((group * 8, LANES), F32),
                vmem((block, width), BF16),
                vmem((pieces_out, half, depth // pieces_out), BF16),
                vmem((pieces_out, half, depth // pieces_out), BF16),
                dma((5,)), dma((2,)),
                dma((group,)), dma((group,)), dma((group,)), dma((group,)),
                dma((halo,)), dma((halo,)),
                dma((group,)), dma((group,)), dma((group,)), dma((group,)),
                dma((pieces_out,)), dma((pieces_out,)),
                pltpu.SemaphoreType.REGULAR((group,)),
            ],
            compiler_params=pltpu.CompilerParams(
                collective_id=0, has_side_effects=True, vmem_limit_bytes=60 * 1024 * 1024
            ),
        )(tokens, w_query, w_key, w_value, w_out)

    in_specs = (
        P(("grp", "sp", "tp"), None),
        P(None, "tp"),
        P(None, "tp"),
        P(None, "tp"),
        P("tp", None),
    )
    out_specs = (P(("grp", "sp", "tp"), None), P("tp", ("grp", "sp")))
    return jax.shard_map(body, mesh=mesh, in_specs=in_specs, out_specs=out_specs, check_vma=False)
```

```python
import functools

import jax
import jax.numpy as jnp
from jax import lax
from jax.experimental import pallas as pl
from jax.experimental.pallas import tpu as pltpu
from jax.sharding import PartitionSpec as P

HEADS = 16
HEAD_DIM = 64
STEPS = 128
REACH = 2048
ALIBI_EXP = 16.0
STRIDE = 16
LANES = 128
MASKED = -1e30
MESH = pl.DeviceIdType.MESH
F32 = jnp.float32
BF16 = jnp.bfloat16


def iota(shape, dim):
    return lax.broadcasted_iota(jnp.int32, shape, dim)


def permuted(m):
    return (m // LANES) * LANES + (m % 8) * STRIDE + (m % LANES) // 8


def kernel(
    rows_sp, tok, wq, wk, wv, wo, own_out, their_out, logs,
    x_in, x_perm, q_w, k_w, v_w, o_w, k_tmp, send_kv, send_q, kv, kv1, q_pk, q_near, q_far, k_far, k_far1,
    bias, far_r, far_m, mid_r, mid_m, o_send, o_recv, l_send, l_recv, l_nat, hid, part, own,
    load_sem, tok_sem, kv_s, kv_r, q_s, q_r, halo_s, halo_r, o_s, o_r, l_s, l_r, part_s, part_r, own_s,
    in_sem, pair_sem, row_sem,
):
    half, depth = tok.shape
    block = 2 * half
    group = q_w.shape[1] // HEAD_DIM
    halo = REACH // block
    far_rows = block // STRIDE
    tile = LANES // far_rows
    tiles = group // tile
    sp, tp = lax.axis_index("sp"), lax.axis_index("tp")
    x = lax.rem(sp, group)
    base = sp - x
    y = sp // group
    up = rows_sp - 1

    def peer(d):
        return {"sp": base + d, "tp": tp}

    partner = {"tp": 1 - tp}

    mine = pl.multiple_of(tp * half, half)
    other_half = pl.multiple_of((1 - tp) * half, half)
    loads = [
        pltpu.make_async_copy(tok, x_in.at[pl.ds(mine, half)], load_sem.at[0]),
        pltpu.make_async_copy(wk, k_w, load_sem.at[1]),
        pltpu.make_async_copy(wv, v_w, load_sem.at[2]),
        pltpu.make_async_copy(wq, q_w, load_sem.at[3]),
        pltpu.make_async_copy(wo, o_w, load_sem.at[4]),
    ]
    for c in loads:
        c.start()

    barrier = pltpu.get_barrier_semaphore()

    @pl.when(tp == 0)
    def _():
        pl.semaphore_signal(barrier, inc=1, device_id=partner, device_id_type=MESH)
        pl.semaphore_wait(pair_sem, 1)
        for d in range(group):
            @pl.when(d < x)
            def _():
                pl.semaphore_signal(barrier, inc=1, device_id=peer(d), device_id_type=MESH)

        @pl.when(y > 0)
        def _():
            pl.semaphore_signal(barrier, inc=1, device_id={"sp": sp - group}, device_id_type=MESH)

    @pl.when(tp == 1)
    def _():
        pl.semaphore_wait(barrier, 1)
        pl.semaphore_signal(pair_sem, inc=1, device_id=partner, device_id_type=MESH)

    loads[0].wait()
    tok_copy = pltpu.make_async_remote_copy(
        src_ref=x_in.at[pl.ds(mine, half)], dst_ref=x_in.at[pl.ds(mine, half)],
        send_sem=tok_sem.at[0], recv_sem=tok_sem.at[1], device_id=partner, device_id_type=MESH)
    tok_copy.start()
    pm, pt = iota((half, half), 0), iota((half, half), 1)
    perm = jnp.where(permuted(pm) == pt, 1.0, 0.0).astype(BF16)
    back = jnp.where(permuted(pt) == pm, 1.0, 0.0).astype(BF16)
    low = iota((half, LANES), 1) < HEAD_DIM
    low_square = iota((LANES, LANES), 1) < HEAD_DIM
    wide = 2 * LANES
    at_once = wide // HEAD_DIM

    def permute(first):
        x_perm[pl.ds(first, half), :] = jnp.dot(perm, x_in[pl.ds(first, half), :], preferred_element_type=F32).astype(BF16)

    def project_kv(first, g):
        rows, cols = pl.ds(first, half), slice(g * wide, (g + 1) * wide)
        k_tmp[...] = jnp.dot(x_perm[rows, :], k_w[:, cols], preferred_element_type=F32)
        v_all = jnp.dot(x_perm[rows, :], v_w[:, cols], preferred_element_type=F32)
        for p in range(2):
            k_p, v_p = k_tmp[:, p * LANES:(p + 1) * LANES], v_all[:, p * LANES:(p + 1) * LANES]
            d = g * at_once + 2 * p
            send_kv[d, rows, :] = jnp.where(low, k_p, pltpu.roll(v_p, HEAD_DIM, 1)).astype(BF16)
            send_kv[d + 1, rows, :] = jnp.where(low, pltpu.roll(k_p, HEAD_DIM, 1), v_p).astype(BF16)

    def project_q(first, g):
        cols = slice(g * wide, (g + 1) * wide)
        rows = pl.ds(pl.multiple_of(first // 2, LANES), LANES)
        q_all = jnp.dot(x_perm[pl.ds(first, half), :], q_w[:, cols], preferred_element_type=F32) * HEAD_DIM ** -0.5
        for p in range(2):
            q_a, q_b = q_all[:LANES, p * LANES:(p + 1) * LANES], q_all[LANES:, p * LANES:(p + 1) * LANES]
            d = g * at_once + 2 * p
            send_q[d, rows, :] = jnp.where(low_square, q_a, pltpu.roll(q_b, HEAD_DIM, 1)).astype(BF16)
            send_q[d + 1, rows, :] = jnp.where(low_square, pltpu.roll(q_a, HEAD_DIM, 1), q_b).astype(BF16)

    def meet_row():
        @pl.when(tp == 0)
        def _():
            greeted = group - 1 - x + jnp.where(y < up, 1, 0)

            @pl.when(greeted > 0)
            def _():
                pl.semaphore_wait(barrier, greeted)

            pl.semaphore_signal(row_sem, inc=1, device_id=partner, device_id_type=MESH)

        @pl.when(tp == 1)
        def _():
            pl.semaphore_wait(row_sem, 1)

        def tell(d, carry):
            pl.semaphore_signal(in_sem.at[x], inc=1, device_id=peer(d), device_id_type=MESH)
            return carry

        lax.fori_loop(x + 1, group, tell, 0)

    pl.when(y == 0)(meet_row)
    permute(mine)
    loads[1].wait()
    loads[2].wait()
    groups = list(reversed(range(group // at_once)))
    for g in groups:
        project_kv(mine, g)

    their_copy = pltpu.make_async_remote_copy(
        src_ref=x_in.at[pl.ds(mine, half)], dst_ref=x_in.at[pl.ds(other_half, half)],
        send_sem=tok_sem.at[0], recv_sem=tok_sem.at[1], device_id=partner, device_id_type=MESH)
    their_copy.wait_recv()
    permute(other_half)

    def kv_copy(d, source):
        return pltpu.make_async_remote_copy(
            src_ref=send_kv.at[d], dst_ref=kv.at[pl.ds(pl.multiple_of(REACH + source * block, block), block)],
            send_sem=kv_s.at[d], recv_sem=kv_r.at[source], device_id=peer(d), device_id_type=MESH)

    def q_copy(d, source):
        return pltpu.make_async_remote_copy(
            src_ref=send_q.at[d], dst_ref=q_pk.at[source],
            send_sem=q_s.at[d], recv_sem=q_r.at[source], device_id=peer(d), device_id_type=MESH)

    own_kv = pltpu.make_async_copy(send_kv.at[x], kv.at[pl.ds(pl.multiple_of(REACH + x * block, block), block)], kv_s.at[x])
    own_q = pltpu.make_async_copy(send_q.at[x], q_pk.at[x], q_s.at[x])

    def offset(i):
        return jnp.where(lax.rem(i, 2) == 1, (i + 1) // 2, group - i // 2)

    def late(d):
        return (d == 0) & (y == 0)

    for n, g in enumerate(groups):
        project_kv(other_half, g)
        if n == 0:
            pl.when(y > 0)(meet_row)

        def send_keys(i, carry):
            d = lax.rem(x + offset(i), group)

            @pl.when((d // at_once == g) & ~late(d))
            def _():
                @pl.when(d < x)
                def _():
                    pl.semaphore_wait(in_sem.at[d], 1)

                kv_copy(d, x).start()

            return carry

        lax.fori_loop(1, group, send_keys, 0)

        @pl.when(x // at_once == g)
        def _():
            own_kv.start()

    loads[3].wait()
    for g in groups:
        project_q(mine, g)
        project_q(other_half, g)
    own_q.start()

    @pl.when((x > 0) & late(0))
    def _():
        pl.semaphore_wait(in_sem.at[0], 1)
        kv_copy(0, x).start()

    def send_queries(i, carry):
        d = lax.rem(x + offset(i), group)

        q_copy(d, x).start()
        return carry

    lax.fori_loop(1, group, send_queries, 0)

    head = (tp * group + x + 1).astype(F32)
    slope = jnp.exp2(jnp.full((LANES, 2 * LANES), -ALIBI_EXP / HEADS, F32) * head)
    row, col = iota((LANES, 2 * LANES), 0), iota((LANES, 2 * LANES), 1)
    near_d = STEPS + permuted(row) - (col // LANES) * LANES - permuted(col % LANES)
    mid_d = STEPS + 4 * (row % 32) + row // 32 - ((col % 64) // 32) * LANES - 4 * (col % 32) - col // 64
    far_d = STEPS + row - col
    before = (col < LANES, (col % 64) < 32, col < LANES)
    for w, (dist, stride) in enumerate(((near_d, 1), (mid_d, 4), (far_d, 16))):
        plain = jnp.where((dist >= 0) & (dist <= STEPS), -slope * (dist * stride).astype(F32), MASKED)
        bias[2 * w] = plain
        bias[2 * w + 1] = jnp.where(before[w] & (y == 0), MASKED, plain)

    @pl.when(y == 0)
    def _():
        kv[pl.ds(0, REACH), :] = jnp.zeros((REACH, LANES), BF16)

    def to_far(ref, first, second, slot, part_index):
        for r in range(STRIDE):
            pair = jnp.concatenate([first[8 * r:8 * r + 8], second[8 * r:8 * r + 8]], axis=0)
            ref[r, pl.ds(pl.multiple_of(far_rows * slot + 16 * part_index, 16), 16), :] = pair.astype(BF16)

    def take_keys(slot):
        for h in range(2):
            first = pl.multiple_of(slot * block + h * half, half)
            values = kv[pl.ds(first, half), :].astype(F32)
            with_ones = jnp.where(low, 1.0, values)
            kv1[pl.ds(first, half), :] = with_ones.astype(BF16)
            to_far(k_far, values[:LANES], values[LANES:], slot, h)
            to_far(k_far1, with_ones[:LANES], with_ones[LANES:], slot, h)

    def take_queries(b):
        for h in range(2):
            values = q_pk[b, h * LANES:(h + 1) * LANES, :].astype(F32)
            first = jnp.where(low_square, values, 0.0)
            second = jnp.where(low_square, pltpu.roll(values, HEAD_DIM, 1), 0.0)
            at = pl.multiple_of(b * block + h * half, half)
            q_near[pl.ds(at, LANES), :] = first.astype(BF16)
            q_near[pl.ds(at + LANES, LANES), :] = second.astype(BF16)
            to_far(q_far, first, second, b, h)

    def halo_copy(b):
        return pltpu.make_async_remote_copy(
            src_ref=kv.at[pl.ds(pl.multiple_of(REACH + b * block, block), block)],
            dst_ref=kv.at[pl.ds(pl.multiple_of((b - (group - halo)) * block, block), block)],
            send_sem=halo_s.at[b - (group - halo)], recv_sem=halo_r.at[b - (group - halo)],
            device_id={"sp": sp + group, "tp": tp}, device_id_type=MESH)

    def pass_on(b):
        @pl.when((b >= group - halo) & (y < up))
        def _():
            halo_copy(b).start()

    own_kv.wait()
    pass_on(x)
    take_keys(x + halo)
    own_q.wait()

    def arrive(i, carry):
        b = lax.rem(x + offset(i), group)

        @pl.when(~late(b))
        def _():
            kv_copy(b, b).wait_recv()
            pass_on(b)
            take_keys(b + halo)

        return carry

    lax.fori_loop(1, group, arrive, 0)

    @pl.when((x > 0) & late(0))
    def _():
        kv_copy(0, 0).wait_recv()
        take_keys(halo)


    def take_halo(i, carry):
        @pl.when(y > 0)
        def _():
            halo_copy(i + group - halo).wait_recv()

        take_keys(i)
        return carry

    def scores(q, keys, which):
        s = lax.dot_general(q, keys, (((1,), (1,)), ((), ())), preferred_element_type=F32) + bias[which]
        m = jnp.max(s, axis=1, keepdims=True)
        return jnp.exp(s - m).astype(BF16), m

    first_row = jnp.where(y == 0, 1, 0)
    eye = iota((LANES, LANES), 0) == iota((LANES, LANES), 1)

    def mid_step(b):
        which = 2 + jnp.where(b == 0, first_row, 0)
        rows_q = pl.ds(pl.multiple_of(far_rows * b, far_rows), far_rows)
        rows_k = pl.ds(pl.multiple_of(far_rows * (b + halo - 1), far_rows), 2 * far_rows)
        for rho in range(4):
            q = jnp.concatenate([q_far[rho + 4 * s, rows_q, :] for s in range(4)], axis=0)
            keys = jnp.concatenate([k_far[rho + 4 * s, rows_k, :] for s in range(4)], axis=0)
            keys1 = jnp.concatenate([k_far1[rho + 4 * s, rows_k, :] for s in range(4)], axis=0)
            w, m = scores(q, keys, which)
            res = jnp.dot(w, keys1, preferred_element_type=F32)
            m_all = jnp.broadcast_to(m, (LANES, LANES))
            for c in range(LANES // 8):
                at = pl.ds(pl.multiple_of(b * block + (c % 4) * LANES + 8 * (rho + 4 * (c // 4)), 8), 8)
                mid_r[at, :] = res[8 * c:8 * c + 8]
                mid_m[at, :] = m_all[8 * c:8 * c + 8]

    def o_copy(d, source):
        return pltpu.make_async_remote_copy(
            src_ref=o_send.at[d], dst_ref=o_recv.at[source],
            send_sem=o_s.at[d], recv_sem=o_r.at[source], device_id=peer(d), device_id_type=MESH)

    def l_copy(d, source):
        return pltpu.make_async_remote_copy(
            src_ref=l_send.at[d], dst_ref=l_recv.at[source],
            send_sem=l_s.at[d], recv_sem=l_r.at[source], device_id=peer(d), device_id_type=MESH)

    def near_step(b):
        for a in range(block // LANES):
            at = pl.ds(pl.multiple_of(b * block + a * LANES, LANES), LANES)
            keys = pl.ds(pl.multiple_of(REACH + b * block + (a - 1) * LANES, LANES), 2 * LANES)
            w, m = scores(q_near[at, :], kv[keys, :], jnp.where(b == 0, first_row, 0) if a == 0 else 0)
            res = jnp.dot(w, kv1[keys, :], preferred_element_type=F32)
            m_m = mid_m[at, :]
            top = jnp.maximum(m_m, m)
            mid_r[at, :] = jnp.exp(m - top) * res + jnp.exp(m_m - top) * mid_r[at, :]
            mid_m[at, :] = top

    def finish(b):
        for h in range(2):
            pieces = []
            for a in (2 * h, 2 * h + 1):
                at = pl.ds(pl.multiple_of(b * block + a * LANES, LANES), LANES)
                m_f, m_m = far_m[at, :], mid_m[at, :]
                top = jnp.maximum(m_f, m_m)
                den = jnp.exp(m_f - top) * far_r[at, :] + jnp.exp(m_m - top) * mid_r[at, :]
                turned = pltpu.roll(den, HEAD_DIM, 1)
                total = jnp.where(low_square, den, turned)
                l_send[b, a, :] = jnp.sum(jnp.where(eye, top + jnp.log(total), 0.0), axis=0)
                pieces.append((den if a % 2 else turned) / total)
            o_send[b, pl.ds(h * LANES, LANES), :] = jnp.where(low_square, pieces[0], pieces[1]).astype(BF16)

        @pl.when(b != x)
        def _():
            o_copy(b, x).start()
            l_copy(b, x).start()

    def far_tile(which_tile):
        first_q = pl.multiple_of(which_tile * LANES, LANES)
        which = 4 + jnp.where(which_tile == 0, first_row, 0)

        def far_step(i, c0):
            for rr in range(8):
                r = 8 * i + rr
                w, m = scores(q_far[r, pl.ds(first_q, LANES), :], k_far[r, pl.ds(first_q, 2 * LANES), :], which)
                res = jnp.dot(w, k_far1[r, pl.ds(first_q, 2 * LANES), :], preferred_element_type=F32)
                m_all = jnp.broadcast_to(m, (LANES, LANES))
                for c in range(LANES // 8):
                    at = pl.ds(pl.multiple_of((which_tile * tile + c // 4) * block + (c % 4) * LANES + 8 * r, 8), 8)
                    far_r[at, :] = res[8 * c:8 * c + 8]
                    far_m[at, :] = m_all[8 * c:8 * c + 8]
            return c0

        lax.fori_loop(0, STRIDE // 8, far_step, 0)

    def close(which_tile):
        far_tile(which_tile)

        def finish_one(j, c):
            finish(which_tile * tile + lax.rem(x + 1 + j, tile))
            return c

        lax.fori_loop(0, tile, finish_one, 0)

    def near_and_mid(b):
        mid_step(b)
        near_step(b)

    def queries(i, carry):
        b = lax.rem(x + jnp.where(i == 0, 0, offset(i)), group)

        @pl.when(b != x)
        def _():
            q_copy(b, b).wait_recv()

        take_queries(b)
        pl.when(b > 0)(lambda: near_and_mid(b))
        return carry

    lax.fori_loop(0, group, queries, 0)

    def close_tile(t, carry):
        which_tile = tiles - 1 - t

        @pl.when(which_tile == 0)
        def _():
            lax.fori_loop(0, halo, take_halo, 0)
            near_and_mid(0)

        close(which_tile)
        return carry

    lax.fori_loop(0, tiles, close_tile, 0)
    own_o = pltpu.make_async_copy(o_send.at[x], o_recv.at[x], o_s.at[x])
    own_l = pltpu.make_async_copy(l_send.at[x], l_recv.at[x], l_s.at[x])
    own_o.start()
    own_l.start()
    own_o.wait()
    own_l.wait()
    loads[4].wait()

    def returned(i, carry):
        b = lax.rem(x + offset(i), group)
        o_copy(b, b).wait_recv()
        l_copy(b, b).wait_recv()
        return carry

    lax.fori_loop(1, group, returned, 0)

    for p in range(group // 2):
        cols = slice(p * LANES, (p + 1) * LANES)
        for h in range(2):
            rows = slice(h * LANES, (h + 1) * LANES)
            even, odd = o_recv[2 * p, rows, :].astype(F32), o_recv[2 * p + 1, rows, :].astype(F32)
            both = jnp.concatenate([jnp.where(low_square, even, pltpu.roll(odd, HEAD_DIM, 1)),
                                    jnp.where(low_square, pltpu.roll(even, HEAD_DIM, 1), odd)], axis=0).astype(BF16)
            hid[h * half:(h + 1) * half, cols] = jnp.dot(back, both, preferred_element_type=F32).astype(BF16)

    pieces_out = part.shape[0]
    step_cols = depth // pieces_out

    def part_copy(i):
        return pltpu.make_async_remote_copy(
            src_ref=part.at[i], dst_ref=their_out.at[:, i * step_cols:(i + 1) * step_cols],
            send_sem=part_s.at[i], recv_sem=part_r.at[i], device_id=partner, device_id_type=MESH)

    def own_copy(i):
        return pltpu.make_async_copy(own.at[i], own_out.at[:, i * step_cols:(i + 1) * step_cols], own_s.at[i])

    for i in range(pieces_out):
        part[i] = jnp.dot(hid[pl.ds(other_half, half), :], o_w[:, i * step_cols:(i + 1) * step_cols],
                          preferred_element_type=F32).astype(BF16)
        part_copy(i).start()

    for i in range(pieces_out):
        own[i] = jnp.dot(hid[pl.ds(mine, half), :], o_w[:, i * step_cols:(i + 1) * step_cols],
                         preferred_element_type=F32).astype(BF16)
        own_copy(i).start()

    flat = jnp.concatenate([l_recv[h] for h in range(group)], axis=0)
    l_nat[...] = jnp.dot(flat, perm[:LANES, :LANES].astype(F32), preferred_element_type=F32, precision=lax.Precision.HIGHEST)
    for a in range(block // LANES):
        logs[:, a * LANES:(a + 1) * LANES] = l_nat[pl.ds(a, group, stride=8), :]

    tok_copy.wait_send()
    for d in range(group):
        @pl.when(d != x)
        def _():
            kv_copy(d, x).wait_send()
            q_copy(d, x).wait_send()
            o_copy(d, x).wait_send()
            l_copy(d, x).wait_send()

    for i in range(halo):
        @pl.when(y < up)
        def _():
            halo_copy(i + group - halo).wait_send()

    for i in range(pieces_out):
        own_copy(i).wait()
        part_copy(i).wait_recv()
        part_copy(i).wait_send()


def solution(mesh):
    def body(tokens, w_query, w_key, w_value, w_out):
        half, depth = tokens.shape
        width = w_query.shape[1]
        block, group = 2 * half, width // HEAD_DIM
        halo = REACH // block
        length = group * block
        far_rows = block // STRIDE
        pieces_out = 4
        vmem = pltpu.VMEM
        dma = pltpu.SemaphoreType.DMA
        anywhere = pl.BlockSpec(memory_space=pl.ANY)
        own, theirs, log_sums = pl.pallas_call(
            functools.partial(kernel, mesh.shape["sp"] // group),
            name="attention_layer",
            out_shape=(
                jax.ShapeDtypeStruct((half, depth), BF16),
                jax.ShapeDtypeStruct((half, depth), BF16),
                jax.ShapeDtypeStruct((group, block), F32),
            ),
            in_specs=[anywhere] * 5,
            out_specs=(anywhere, anywhere, pl.BlockSpec(memory_space=vmem)),
            scratch_shapes=[
                vmem((block, depth), BF16),
                vmem((block, depth), BF16),
                vmem((depth, width), BF16),
                vmem((depth, width), BF16),
                vmem((depth, width), BF16),
                vmem((width, depth), BF16),
                vmem((half, 2 * LANES), F32),
                vmem((group, block, LANES), BF16),
                vmem((group, half, LANES), BF16),
                vmem((REACH + length, LANES), BF16),
                vmem((REACH + length, LANES), BF16),
                vmem((group, half, LANES), BF16),
                vmem((length, LANES), BF16),
                vmem((STRIDE, group * far_rows, LANES), BF16),
                vmem((STRIDE, (halo + group) * far_rows, LANES), BF16),
                vmem((STRIDE, (halo + group) * far_rows, LANES), BF16),
                vmem((6, LANES, 2 * LANES), F32),
                vmem((length, LANES), F32),
                vmem((length, LANES), F32),
                vmem((length, LANES), F32),
                vmem((length, LANES), F32),
                vmem((group, half, LANES), BF16),
                vmem((group, half, LANES), BF16),
                vmem((group, 8, LANES), F32),
                vmem((group, 8, LANES), F32),
                vmem((group * 8, LANES), F32),
                vmem((block, width), BF16),
                vmem((pieces_out, half, depth // pieces_out), BF16),
                vmem((pieces_out, half, depth // pieces_out), BF16),
                dma((5,)), dma((2,)),
                dma((group,)), dma((group,)), dma((group,)), dma((group,)),
                dma((halo,)), dma((halo,)),
                dma((group,)), dma((group,)), dma((group,)), dma((group,)),
                dma((pieces_out,)), dma((pieces_out,)), dma((pieces_out,)),
                pltpu.SemaphoreType.REGULAR((group,)), pltpu.SemaphoreType.REGULAR, pltpu.SemaphoreType.REGULAR,
            ],
            compiler_params=pltpu.CompilerParams(
                collective_id=0, has_side_effects=True, vmem_limit_bytes=60 * 1024 * 1024
            ),
        )(tokens, w_query, w_key, w_value, w_out)
        return (own.astype(F32) + theirs.astype(F32)).astype(BF16), log_sums

    in_specs = (
        P(("grp", "sp", "tp"), None),
        P(None, "tp"),
        P(None, "tp"),
        P(None, "tp"),
        P("tp", None),
    )
    out_specs = (P(("grp", "sp", "tp"), None), P("tp", ("grp", "sp")))
    return jax.shard_map(body, mesh=mesh, in_specs=in_specs, out_specs=out_specs, check_vma=False)
```

```python
import functools

import jax
import jax.numpy as jnp
from jax import lax
from jax.experimental import pallas as pl
from jax.experimental.pallas import tpu as pltpu
from jax.sharding import PartitionSpec as P

HEADS = 16
HEAD_DIM = 64
STEPS = 128
REACH = 2048
ALIBI_EXP = 16.0
STRIDE = 16
LANES = 128
MASKED = -1e30
MESH = pl.DeviceIdType.MESH
F32 = jnp.float32
BF16 = jnp.bfloat16


def iota(shape, dim):
    return lax.broadcasted_iota(jnp.int32, shape, dim)


def permuted(m):
    return (m // LANES) * LANES + (m % 8) * STRIDE + (m % LANES) // 8


def kernel(
    rows_sp, tok, wq, wk, wv, wo, own_out, their_out, logs,
    x_in, x_perm, q_w, k_w, v_w, o_w, k_tmp, send_kv, send_q, kv, kv1, q_pk, q_near, q_far, k_far, k_far1,
    bias, far_r, far_m, mid_r, mid_m, o_send, o_recv, l_send, l_recv, l_nat, hid, part, own,
    load_sem, tok_sem, kv_s, kv_r, q_s, q_r, halo_s, halo_r, o_s, o_r, l_s, l_r, part_s, part_r, own_s,
    in_sem, pair_sem, row_sem,
):
    half, depth = tok.shape
    block = 2 * half
    group = q_w.shape[1] // HEAD_DIM
    halo = REACH // block
    far_rows = block // STRIDE
    tile = LANES // far_rows
    tiles = group // tile
    sp, tp = lax.axis_index("sp"), lax.axis_index("tp")
    x = lax.rem(sp, group)
    base = sp - x
    y = sp // group
    up = rows_sp - 1

    def peer(d):
        return {"sp": base + d, "tp": tp}

    partner = {"tp": 1 - tp}

    mine = pl.multiple_of(tp * half, half)
    other_half = pl.multiple_of((1 - tp) * half, half)
    loads = [
        pltpu.make_async_copy(tok, x_in.at[pl.ds(mine, half)], load_sem.at[0]),
        pltpu.make_async_copy(wk, k_w, load_sem.at[1]),
        pltpu.make_async_copy(wv, v_w, load_sem.at[2]),
        pltpu.make_async_copy(wq, q_w, load_sem.at[3]),
        pltpu.make_async_copy(wo, o_w, load_sem.at[4]),
    ]
    for c in loads:
        c.start()

    barrier = pltpu.get_barrier_semaphore()

    @pl.when(tp == 0)
    def _():
        pl.semaphore_signal(barrier, inc=1, device_id=partner, device_id_type=MESH)
        pl.semaphore_wait(pair_sem, 1)
        for d in range(group):
            @pl.when(d < x)
            def _():
                pl.semaphore_signal(barrier, inc=1, device_id=peer(d), device_id_type=MESH)

        @pl.when(y > 0)
        def _():
            pl.semaphore_signal(barrier, inc=1, device_id={"sp": sp - group}, device_id_type=MESH)

    @pl.when(tp == 1)
    def _():
        pl.semaphore_wait(barrier, 1)
        pl.semaphore_signal(pair_sem, inc=1, device_id=partner, device_id_type=MESH)

    loads[0].wait()
    tok_copy = pltpu.make_async_remote_copy(
        src_ref=x_in.at[pl.ds(mine, half)], dst_ref=x_in.at[pl.ds(mine, half)],
        send_sem=tok_sem.at[0], recv_sem=tok_sem.at[1], device_id=partner, device_id_type=MESH)
    tok_copy.start()
    pm, pt = iota((half, half), 0), iota((half, half), 1)
    perm = jnp.where(permuted(pm) == pt, 1.0, 0.0).astype(BF16)
    back = jnp.where(permuted(pt) == pm, 1.0, 0.0).astype(BF16)
    low = iota((half, LANES), 1) < HEAD_DIM
    low_square = iota((LANES, LANES), 1) < HEAD_DIM
    wide = 2 * LANES
    at_once = wide // HEAD_DIM

    def permute(first):
        x_perm[pl.ds(first, half), :] = jnp.dot(perm, x_in[pl.ds(first, half), :], preferred_element_type=F32).astype(BF16)

    def project_kv(first, g):
        rows, cols = pl.ds(first, half), slice(g * wide, (g + 1) * wide)
        k_tmp[...] = jnp.dot(x_perm[rows, :], k_w[:, cols], preferred_element_type=F32)
        v_all = jnp.dot(x_perm[rows, :], v_w[:, cols], preferred_element_type=F32)
        for p in range(2):
            k_p, v_p = k_tmp[:, p * LANES:(p + 1) * LANES], v_all[:, p * LANES:(p + 1) * LANES]
            d = g * at_once + 2 * p
            send_kv[d, rows, :] = jnp.where(low, k_p, pltpu.roll(v_p, HEAD_DIM, 1)).astype(BF16)
            send_kv[d + 1, rows, :] = jnp.where(low, pltpu.roll(k_p, HEAD_DIM, 1), v_p).astype(BF16)

    def project_q(first, g):
        cols = slice(g * wide, (g + 1) * wide)
        rows = pl.ds(pl.multiple_of(first // 2, LANES), LANES)
        q_all = jnp.dot(x_perm[pl.ds(first, half), :], q_w[:, cols], preferred_element_type=F32) * HEAD_DIM ** -0.5
        for p in range(2):
            q_a, q_b = q_all[:LANES, p * LANES:(p + 1) * LANES], q_all[LANES:, p * LANES:(p + 1) * LANES]
            d = g * at_once + 2 * p
            send_q[d, rows, :] = jnp.where(low_square, q_a, pltpu.roll(q_b, HEAD_DIM, 1)).astype(BF16)
            send_q[d + 1, rows, :] = jnp.where(low_square, pltpu.roll(q_a, HEAD_DIM, 1), q_b).astype(BF16)

    def meet_row():
        @pl.when(tp == 0)
        def _():
            greeted = group - 1 - x + jnp.where(y < up, 1, 0)

            @pl.when(greeted > 0)
            def _():
                pl.semaphore_wait(barrier, greeted)

            pl.semaphore_signal(row_sem, inc=1, device_id=partner, device_id_type=MESH)

        @pl.when(tp == 1)
        def _():
            pl.semaphore_wait(row_sem, 1)

        def tell(d, carry):
            pl.semaphore_signal(in_sem.at[x], inc=1, device_id=peer(d), device_id_type=MESH)
            return carry

        lax.fori_loop(x + 1, group, tell, 0)

    pl.when(y == 0)(meet_row)
    def kv_copy(d, source, h):
        return pltpu.make_async_remote_copy(
            src_ref=send_kv.at[d, pl.ds(pl.multiple_of(h * half, half), half)],
            dst_ref=kv.at[pl.ds(pl.multiple_of(REACH + source * block + h * half, half), half)],
            send_sem=kv_s.at[2 * d + h], recv_sem=kv_r.at[2 * source + h], device_id=peer(d), device_id_type=MESH)

    def q_copy(d, source):
        return pltpu.make_async_remote_copy(
            src_ref=send_q.at[d], dst_ref=q_pk.at[source],
            send_sem=q_s.at[d], recv_sem=q_r.at[source], device_id=peer(d), device_id_type=MESH)

    own_kv = pltpu.make_async_copy(send_kv.at[x], kv.at[pl.ds(pl.multiple_of(REACH + x * block, block), block)], kv_s.at[2 * x])
    own_q = pltpu.make_async_copy(send_q.at[x], q_pk.at[x], q_s.at[x])

    def offset(i):
        return jnp.where(lax.rem(i, 2) == 1, (i + 1) // 2, group - i // 2)

    def late(d):
        return (d == 0) & (y == 0)

    def send_keys(h, first_time):
        def one(i, carry):
            d = lax.rem(x + offset(i), group)

            @pl.when(~late(d))
            def _():
                if first_time:
                    @pl.when(d < x)
                    def _():
                        pl.semaphore_wait(in_sem.at[d], 1)

                kv_copy(d, x, h).start()

            return carry

        lax.fori_loop(1, group, one, 0)

    permute(mine)
    loads[1].wait()
    loads[2].wait()
    groups = range(group // at_once)
    for g in groups:
        project_kv(mine, g)
    pl.when(y > 0)(meet_row)
    send_keys(tp, True)
    pltpu.make_async_remote_copy(
        src_ref=x_in.at[pl.ds(mine, half)], dst_ref=x_in.at[pl.ds(other_half, half)],
        send_sem=tok_sem.at[0], recv_sem=tok_sem.at[1], device_id=partner, device_id_type=MESH).wait_recv()
    permute(other_half)
    for g in groups:
        project_kv(other_half, g)
    send_keys(1 - tp, False)
    own_kv.start()

    loads[3].wait()
    for g in groups:
        project_q(mine, g)
        project_q(other_half, g)
    own_q.start()

    @pl.when((x > 0) & late(0))
    def _():
        pl.semaphore_wait(in_sem.at[0], 1)
        kv_copy(0, x, tp).start()
        kv_copy(0, x, 1 - tp).start()

    def send_queries(i, carry):
        d = lax.rem(x + offset(i), group)

        q_copy(d, x).start()
        return carry

    lax.fori_loop(1, group, send_queries, 0)

    head = (tp * group + x + 1).astype(F32)
    slope = jnp.exp2(jnp.full((LANES, 2 * LANES), -ALIBI_EXP / HEADS, F32) * head)
    row, col = iota((LANES, 2 * LANES), 0), iota((LANES, 2 * LANES), 1)
    near_d = STEPS + permuted(row) - (col // LANES) * LANES - permuted(col % LANES)
    mid_d = STEPS + 4 * (row % 32) + row // 32 - ((col % 64) // 32) * LANES - 4 * (col % 32) - col // 64
    far_d = STEPS + row - col
    before = (col < LANES, (col % 64) < 32, col < LANES)
    for w, (dist, stride) in enumerate(((near_d, 1), (mid_d, 4), (far_d, 16))):
        plain = jnp.where((dist >= 0) & (dist <= STEPS), -slope * (dist * stride).astype(F32), MASKED)
        bias[2 * w] = plain
        bias[2 * w + 1] = jnp.where(before[w] & (y == 0), MASKED, plain)

    @pl.when(y == 0)
    def _():
        kv[pl.ds(0, REACH), :] = jnp.zeros((REACH, LANES), BF16)

    def to_far(ref, first, second, slot, part_index):
        for r in range(STRIDE):
            pair = jnp.concatenate([first[8 * r:8 * r + 8], second[8 * r:8 * r + 8]], axis=0)
            ref[r, pl.ds(pl.multiple_of(far_rows * slot + 16 * part_index, 16), 16), :] = pair.astype(BF16)

    def take_keys(slot):
        for h in range(2):
            first = pl.multiple_of(slot * block + h * half, half)
            values = kv[pl.ds(first, half), :].astype(F32)
            with_ones = jnp.where(low, 1.0, values)
            kv1[pl.ds(first, half), :] = with_ones.astype(BF16)
            to_far(k_far, values[:LANES], values[LANES:], slot, h)
            to_far(k_far1, with_ones[:LANES], with_ones[LANES:], slot, h)

    def take_queries(b):
        for h in range(2):
            values = q_pk[b, h * LANES:(h + 1) * LANES, :].astype(F32)
            first = jnp.where(low_square, values, 0.0)
            second = jnp.where(low_square, pltpu.roll(values, HEAD_DIM, 1), 0.0)
            at = pl.multiple_of(b * block + h * half, half)
            q_near[pl.ds(at, LANES), :] = first.astype(BF16)
            q_near[pl.ds(at + LANES, LANES), :] = second.astype(BF16)
            to_far(q_far, first, second, b, h)

    def halo_copy(b):
        return pltpu.make_async_remote_copy(
            src_ref=kv.at[pl.ds(pl.multiple_of(REACH + b * block, block), block)],
            dst_ref=kv.at[pl.ds(pl.multiple_of((b - (group - halo)) * block, block), block)],
            send_sem=halo_s.at[b - (group - halo)], recv_sem=halo_r.at[b - (group - halo)],
            device_id={"sp": sp + group, "tp": tp}, device_id_type=MESH)

    def pass_on(b):
        @pl.when((b >= group - halo) & (y < up))
        def _():
            halo_copy(b).start()

    own_kv.wait()
    pass_on(x)
    take_keys(x + halo)
    own_q.wait()

    def arrive(i, carry):
        b = lax.rem(x + offset(i), group)

        @pl.when(~late(b))
        def _():
            kv_copy(b, b, 0).wait_recv()
            kv_copy(b, b, 1).wait_recv()
            pass_on(b)
            take_keys(b + halo)

        return carry

    lax.fori_loop(1, group, arrive, 0)


    def take_halo(i, carry):
        @pl.when(y > 0)
        def _():
            halo_copy(i + group - halo).wait_recv()

        take_keys(i)
        return carry

    def scores(q, keys, which):
        s = lax.dot_general(q, keys, (((1,), (1,)), ((), ())), preferred_element_type=F32) + bias[which]
        m = jnp.max(s, axis=1, keepdims=True)
        return jnp.exp(s - m).astype(BF16), m

    first_row = jnp.where(y == 0, 1, 0)
    eye = iota((LANES, LANES), 0) == iota((LANES, LANES), 1)

    def mid_step(b):
        which = 2 + jnp.where(b == 0, first_row, 0)
        rows_q = pl.ds(pl.multiple_of(far_rows * b, far_rows), far_rows)
        rows_k = pl.ds(pl.multiple_of(far_rows * (b + halo - 1), far_rows), 2 * far_rows)
        for rho in range(4):
            q = jnp.concatenate([q_far[rho + 4 * s, rows_q, :] for s in range(4)], axis=0)
            keys = jnp.concatenate([k_far[rho + 4 * s, rows_k, :] for s in range(4)], axis=0)
            keys1 = jnp.concatenate([k_far1[rho + 4 * s, rows_k, :] for s in range(4)], axis=0)
            w, m = scores(q, keys, which)
            res = jnp.dot(w, keys1, preferred_element_type=F32)
            m_all = jnp.broadcast_to(m, (LANES, LANES))
            for c in range(LANES // 8):
                at = pl.ds(pl.multiple_of(b * block + (c % 4) * LANES + 8 * (rho + 4 * (c // 4)), 8), 8)
                mid_r[at, :] = res[8 * c:8 * c + 8]
                mid_m[at, :] = m_all[8 * c:8 * c + 8]

    def o_copy(d, source):
        return pltpu.make_async_remote_copy(
            src_ref=o_send.at[d], dst_ref=o_recv.at[source],
            send_sem=o_s.at[d], recv_sem=o_r.at[source], device_id=peer(d), device_id_type=MESH)

    def l_copy(d, source):
        return pltpu.make_async_remote_copy(
            src_ref=l_send.at[d], dst_ref=l_recv.at[source],
            send_sem=l_s.at[d], recv_sem=l_r.at[source], device_id=peer(d), device_id_type=MESH)

    def near_step(b):
        for a in range(block // LANES):
            at = pl.ds(pl.multiple_of(b * block + a * LANES, LANES), LANES)
            keys = pl.ds(pl.multiple_of(REACH + b * block + (a - 1) * LANES, LANES), 2 * LANES)
            w, m = scores(q_near[at, :], kv[keys, :], jnp.where(b == 0, first_row, 0) if a == 0 else 0)
            res = jnp.dot(w, kv1[keys, :], preferred_element_type=F32)
            m_m = mid_m[at, :]
            top = jnp.maximum(m_m, m)
            mid_r[at, :] = jnp.exp(m - top) * res + jnp.exp(m_m - top) * mid_r[at, :]
            mid_m[at, :] = top

    def finish(b):
        for h in range(2):
            pieces = []
            for a in (2 * h, 2 * h + 1):
                at = pl.ds(pl.multiple_of(b * block + a * LANES, LANES), LANES)
                m_f, m_m = far_m[at, :], mid_m[at, :]
                top = jnp.maximum(m_f, m_m)
                den = jnp.exp(m_f - top) * far_r[at, :] + jnp.exp(m_m - top) * mid_r[at, :]
                turned = pltpu.roll(den, HEAD_DIM, 1)
                total = jnp.where(low_square, den, turned)
                l_send[b, a, :] = jnp.sum(jnp.where(eye, top + jnp.log(total), 0.0), axis=0)
                pieces.append((den if a % 2 else turned) / total)
            o_send[b, pl.ds(h * LANES, LANES), :] = jnp.where(low_square, pieces[0], pieces[1]).astype(BF16)

        @pl.when(b != x)
        def _():
            o_copy(b, x).start()
            l_copy(b, x).start()

    def far_tile(which_tile):
        first_q = pl.multiple_of(which_tile * LANES, LANES)
        which = 4 + jnp.where(which_tile == 0, first_row, 0)

        def far_step(i, c0):
            for rr in range(8):
                r = 8 * i + rr
                w, m = scores(q_far[r, pl.ds(first_q, LANES), :], k_far[r, pl.ds(first_q, 2 * LANES), :], which)
                res = jnp.dot(w, k_far1[r, pl.ds(first_q, 2 * LANES), :], preferred_element_type=F32)
                m_all = jnp.broadcast_to(m, (LANES, LANES))
                for c in range(LANES // 8):
                    at = pl.ds(pl.multiple_of((which_tile * tile + c // 4) * block + (c % 4) * LANES + 8 * r, 8), 8)
                    far_r[at, :] = res[8 * c:8 * c + 8]
                    far_m[at, :] = m_all[8 * c:8 * c + 8]
            return c0

        lax.fori_loop(0, STRIDE // 8, far_step, 0)

    def close(which_tile):
        far_tile(which_tile)

        def finish_one(j, c):
            finish(which_tile * tile + lax.rem(x + 1 + j, tile))
            return c

        lax.fori_loop(0, tile, finish_one, 0)

    def near_and_mid(b):
        mid_step(b)
        near_step(b)

    def queries(i, carry):
        b = lax.rem(x + jnp.where(i == 0, 0, offset(i)), group)

        @pl.when((b == x) | ~late(b))
        def _():
            @pl.when(b != x)
            def _():
                q_copy(b, b).wait_recv()

            take_queries(b)
            pl.when((b > 0) & ((x == 0) | ~late(b - 1)))(lambda: near_and_mid(b))

        return carry

    lax.fori_loop(0, group, queries, 0)

    @pl.when((x > 0) & late(0))
    def _():
        kv_copy(0, 0, 0).wait_recv()
        kv_copy(0, 0, 1).wait_recv()
        take_keys(halo)
        near_and_mid(1)

    def close_tile(t, carry):
        which_tile = lax.rem(jnp.where((y == 1) & (x == 0), tiles - 1, 0) + t, tiles)

        @pl.when(which_tile == 0)
        def _():
            lax.fori_loop(0, halo, take_halo, 0)

            @pl.when((x > 0) & late(0))
            def _():
                q_copy(0, 0).wait_recv()
                take_queries(0)

            near_and_mid(0)

        close(which_tile)
        return carry

    lax.fori_loop(0, tiles, close_tile, 0)
    own_o = pltpu.make_async_copy(o_send.at[x], o_recv.at[x], o_s.at[x])
    own_l = pltpu.make_async_copy(l_send.at[x], l_recv.at[x], l_s.at[x])
    own_o.start()
    own_l.start()
    own_o.wait()
    own_l.wait()
    loads[4].wait()

    def returned(i, carry):
        b = lax.rem(x + offset(i), group)
        o_copy(b, b).wait_recv()
        l_copy(b, b).wait_recv()
        return carry

    lax.fori_loop(1, group, returned, 0)

    for p in range(group // 2):
        cols = slice(p * LANES, (p + 1) * LANES)
        for h in range(2):
            rows = slice(h * LANES, (h + 1) * LANES)
            even, odd = o_recv[2 * p, rows, :].astype(F32), o_recv[2 * p + 1, rows, :].astype(F32)
            both = jnp.concatenate([jnp.where(low_square, even, pltpu.roll(odd, HEAD_DIM, 1)),
                                    jnp.where(low_square, pltpu.roll(even, HEAD_DIM, 1), odd)], axis=0).astype(BF16)
            hid[h * half:(h + 1) * half, cols] = jnp.dot(back, both, preferred_element_type=F32).astype(BF16)

    pieces_out = part.shape[0]
    step_cols = depth // pieces_out

    def part_copy(i):
        return pltpu.make_async_remote_copy(
            src_ref=part.at[i], dst_ref=their_out.at[:, i * step_cols:(i + 1) * step_cols],
            send_sem=part_s.at[i], recv_sem=part_r.at[i], device_id=partner, device_id_type=MESH)

    def own_copy(i):
        return pltpu.make_async_copy(own.at[i], own_out.at[:, i * step_cols:(i + 1) * step_cols], own_s.at[i])

    for i in range(pieces_out):
        part[i] = jnp.dot(hid[pl.ds(other_half, half), :], o_w[:, i * step_cols:(i + 1) * step_cols],
                          preferred_element_type=F32).astype(BF16)
        part_copy(i).start()

    for i in range(pieces_out):
        own[i] = jnp.dot(hid[pl.ds(mine, half), :], o_w[:, i * step_cols:(i + 1) * step_cols],
                         preferred_element_type=F32).astype(BF16)
        own_copy(i).start()

    flat = jnp.concatenate([l_recv[h] for h in range(group)], axis=0)
    l_nat[...] = jnp.dot(flat, perm[:LANES, :LANES].astype(F32), preferred_element_type=F32, precision=lax.Precision.HIGHEST)
    for a in range(block // LANES):
        logs[:, a * LANES:(a + 1) * LANES] = l_nat[pl.ds(a, group, stride=8), :]

    tok_copy.wait_send()
    for d in range(group):
        @pl.when(d != x)
        def _():
            kv_copy(d, x, 0).wait_send()
            kv_copy(d, x, 1).wait_send()
            q_copy(d, x).wait_send()
            o_copy(d, x).wait_send()
            l_copy(d, x).wait_send()

    for i in range(halo):
        @pl.when(y < up)
        def _():
            halo_copy(i + group - halo).wait_send()

    for i in range(pieces_out):
        own_copy(i).wait()
        part_copy(i).wait_recv()
        part_copy(i).wait_send()


def solution(mesh):
    def body(tokens, w_query, w_key, w_value, w_out):
        half, depth = tokens.shape
        width = w_query.shape[1]
        block, group = 2 * half, width // HEAD_DIM
        halo = REACH // block
        length = group * block
        far_rows = block // STRIDE
        pieces_out = 4
        vmem = pltpu.VMEM
        dma = pltpu.SemaphoreType.DMA
        anywhere = pl.BlockSpec(memory_space=pl.ANY)
        own, theirs, log_sums = pl.pallas_call(
            functools.partial(kernel, mesh.shape["sp"] // group),
            name="attention_layer",
            out_shape=(
                jax.ShapeDtypeStruct((half, depth), BF16),
                jax.ShapeDtypeStruct((half, depth), BF16),
                jax.ShapeDtypeStruct((group, block), F32),
            ),
            in_specs=[pl.BlockSpec(memory_space=pltpu.MemorySpace.HBM)] * 5,
            out_specs=(anywhere, anywhere, pl.BlockSpec(memory_space=vmem)),
            scratch_shapes=[
                vmem((block, depth), BF16),
                vmem((block, depth), BF16),
                vmem((depth, width), BF16),
                vmem((depth, width), BF16),
                vmem((depth, width), BF16),
                vmem((width, depth), BF16),
                vmem((half, 2 * LANES), F32),
                vmem((group, block, LANES), BF16),
                vmem((group, half, LANES), BF16),
                vmem((REACH + length, LANES), BF16),
                vmem((REACH + length, LANES), BF16),
                vmem((group, half, LANES), BF16),
                vmem((length, LANES), BF16),
                vmem((STRIDE, group * far_rows, LANES), BF16),
                vmem((STRIDE, (halo + group) * far_rows, LANES), BF16),
                vmem((STRIDE, (halo + group) * far_rows, LANES), BF16),
                vmem((6, LANES, 2 * LANES), F32),
                vmem((length, LANES), F32),
                vmem((length, LANES), F32),
                vmem((length, LANES), F32),
                vmem((length, LANES), F32),
                vmem((group, half, LANES), BF16),
                vmem((group, half, LANES), BF16),
                vmem((group, 8, LANES), F32),
                vmem((group, 8, LANES), F32),
                vmem((group * 8, LANES), F32),
                vmem((block, width), BF16),
                vmem((pieces_out, half, depth // pieces_out), BF16),
                vmem((pieces_out, half, depth // pieces_out), BF16),
                dma((5,)), dma((2,)),
                dma((2 * group,)), dma((2 * group,)), dma((group,)), dma((group,)),
                dma((halo,)), dma((halo,)),
                dma((group,)), dma((group,)), dma((group,)), dma((group,)),
                dma((pieces_out,)), dma((pieces_out,)), dma((pieces_out,)),
                pltpu.SemaphoreType.REGULAR((group,)), pltpu.SemaphoreType.REGULAR, pltpu.SemaphoreType.REGULAR,
            ],
            compiler_params=pltpu.CompilerParams(
                collective_id=0, has_side_effects=True, vmem_limit_bytes=51 * 1024 * 1024
            ),
        )(tokens, w_query, w_key, w_value, w_out)
        return (own.astype(F32) + theirs.astype(F32)).astype(BF16), log_sums

    in_specs = (
        P(("grp", "sp", "tp"), None),
        P(None, "tp"),
        P(None, "tp"),
        P(None, "tp"),
        P("tp", None),
    )
    out_specs = (P(("grp", "sp", "tp"), None), P("tp", ("grp", "sp")))
    return jax.shard_map(body, mesh=mesh, in_specs=in_specs, out_specs=out_specs, check_vma=False)
```
